128 devices in a mesh: fs: 16 (over z, x), tp: 8 (over y, core).
Axes of the slice: x: 4, y: 4, z: 4, core: 2. Of those that a mesh axis runs over, the one named last changes fastest.
Arguments:
- tokens: bfloat16 [16384, 2048], P(('fs', 'tp')), may hold values from -6 to 6
- gate_weight: bfloat16 [2048, 6144], P('fs', 'tp'), may hold values from -0.125 to 0.125
- value_weight: bfloat16 [2048, 6144], P('fs', 'tp'), may hold values from -0.125 to 0.125
- gate_taps: float32 [3, 6144], P(None, 'tp'), may hold values from -3.5 to 3.5
- value_taps: float32 [3, 6144], P(None, 'tp'), may hold values from -3.5 to 3.5
- down_weight: bfloat16 [6144, 2048], P('tp', 'fs'), may hold values from -0.078125 to 0.078125
- norm_gain: float32 [2048], replicated, may hold values from 0.1 to 1.9
- norm_shift: float32 [2048], replicated, may hold values from -3 to 3
Outputs:
- mixed: bfloat16 [16384, 2048], P(('fs', 'tp'))
The draws below stay inside these ranges and needn't reach their ends.
All inputs are finite; a program needn't handle non-finite values.
Results may differ from the reference program's by a relative error of at most 0.017.
Values may be sent and summed in bfloat16 or wider, within the bound.
No kernel may reach another device: no remote copies, remote signals or barrier semaphores. Data moves between devices by JAX's collectives and lax.ppermute only.
A program may use at most 256 MiB of HBM per device.

```python
import jax
import jax.numpy as jnp
from jax import lax

D = 2048
FF = 6144
TAPS = 3
TOK_DEV = 128
TOKENS = 16384
N_FS = 16
N_TP = 8


def block_scale(own_key, shape, cuts, smallest, top_value):
    level = 1.0
    for position, blocks in cuts:
        draws = jax.random.uniform(jax.random.fold_in(jax.random.fold_in(own_key, 6), position), (blocks,), jnp.float32, smallest / len(cuts), top_value / len(cuts))
        level = level * jnp.repeat(jnp.exp(draws), shape[position] // blocks).reshape((-1,) + (1,) * (len(shape) - 1 - position))
    return level


def bell_draw(stream_key, shape, width, reach, shards=(), dtype=jnp.bfloat16):
    array = width * jax.random.normal(stream_key, shape, jnp.float32)
    if shards:
        array = array * block_scale(stream_key, shape, shards, -0.22, 0.18)
    return jnp.clip(array, -reach, reach).astype(dtype)


def setup_inputs(seed: int = 0) -> dict:
    arg_keys = jax.random.split(jax.random.key(seed), 9)
    tokens = bell_draw(arg_keys[0], (TOKENS, D), 1.0, 6.0, ((0, 128),))
    gate_weight = bell_draw(arg_keys[1], (D, FF), D ** -0.5, 0.125, ((0, 16), (1, 8)))
    value_weight = bell_draw(arg_keys[2], (D, FF), D ** -0.5, 0.125, ((0, 16), (1, 8)))
    gate_taps = bell_draw(arg_keys[3], (TAPS, FF), TAPS ** -0.5, 3.5, ((1, 8),), jnp.float32)
    value_taps = bell_draw(arg_keys[4], (TAPS, FF), TAPS ** -0.5, 3.5, ((1, 8),), jnp.float32)
    down_weight = bell_draw(arg_keys[5], (FF, D), FF ** -0.5, 0.078125, ((0, 8), (1, 16)))
    norm_gain = jnp.clip(1.0 + 0.18 * jax.random.normal(arg_keys[6], (D,), jnp.float32), 0.1, 1.9)
    norm_shift = bell_draw(arg_keys[7], (D,), 0.5, 3.0, (), jnp.float32)
    return dict(tokens=tokens, gate_weight=gate_weight, value_weight=value_weight, gate_taps=gate_taps, value_taps=value_taps, down_weight=down_weight, norm_gain=norm_gain, norm_shift=norm_shift)


def causal_mix(pre, kernel_taps):
    leading = jnp.zeros((2, pre.shape[1]), jnp.float32)
    padded = jnp.concatenate([leading, pre.astype(jnp.float32)], axis=0)
    length = pre.shape[0]
    return kernel_taps[0] * padded[0:length] + kernel_taps[1] * padded[1:length + 1] + kernel_taps[2] * padded[2:length + 2]

def one_sequence(rows, gate_weight, value_weight, gate_taps, value_taps, down_weight, norm_gain, norm_shift):
    gate_pre = jnp.dot(rows, gate_weight, preferred_element_type=jnp.float32).astype(jnp.bfloat16)
    value_pre = jnp.dot(rows, value_weight, preferred_element_type=jnp.float32).astype(jnp.bfloat16)
    gate_mix = causal_mix(gate_pre, gate_taps)
    value_mix = causal_mix(value_pre, value_taps)
    hidden = (jax.nn.gelu(gate_mix, approximate=False) * value_mix).astype(jnp.bfloat16)
    length = rows.shape[0]
    block_cols = FF // N_TP
    hidden_blocks = hidden.reshape(length, N_TP, block_cols).astype(jnp.float32)
    down_blocks = down_weight.reshape(N_TP, block_cols, D).astype(jnp.float32)
    partials = jnp.einsum('lkf,kfd->kld', hidden_blocks, down_blocks).astype(jnp.bfloat16)
    summed = lax.optimization_barrier(jnp.sum(partials.astype(jnp.float32), axis=0))
    average = lax.optimization_barrier(jnp.mean(summed, axis=1, keepdims=True))
    centered = summed - average
    variance = lax.optimization_barrier(jnp.mean(centered * centered, axis=1, keepdims=True))
    normed = centered * lax.rsqrt(variance + 1e-05) * norm_gain + norm_shift
    return normed.astype(jnp.bfloat16)

def reference(tokens, gate_weight, value_weight, gate_taps, value_taps, down_weight, norm_gain, norm_shift):
    length = TOK_DEV * N_TP
    grouped = tokens.reshape(N_FS, length, D)
    result = lax.map(lambda rows: one_sequence(rows, gate_weight, value_weight, gate_taps, value_taps, down_weight, norm_gain, norm_shift), grouped)
    return result.reshape(N_FS * length, D)
```

```python
import functools

import jax
import jax.numpy as jnp
from jax import lax
from jax.experimental import pallas as pl
from jax.experimental.pallas import tpu as pltpu
from jax.sharding import PartitionSpec as P

AX = ("fs", "tp")
ANY = pl.BlockSpec(memory_space=pl.ANY)
VMEM = pl.BlockSpec(memory_space=pltpu.VMEM)
SMEM = pl.BlockSpec(memory_space=pltpu.SMEM)
BF = jnp.bfloat16
F32 = jnp.float32

OFFSETS = (
    (0, 0), (0, -1), (0, 1), (-1, 0), (1, 0), (2, 0),
    (-1, 2), (1, 2), (-1, -1), (-1, 1), (1, -1), (1, 1),
    (0, 2), (2, 2), (2, -1), (2, 1),
)


def pairs(step):
    out = []
    for z in range(4):
        for x in range(4):
            for y in range(4):
                for c in range(2):
                    tx, ty, tz, tc = step(x, y, z, c)
                    out.append((
                        (z * 4 + x) * 8 + y * 2 + c,
                        ((tz % 4) * 4 + tx % 4) * 8 + (ty % 4) * 2 + tc,
                    ))
    return out


def along(first, d, flip):
    def step(x, y, z, c):
        even = ((x + z) % 2 == 0) != flip
        return (x + d, y, z, c) if even == first else (x, y, z + d, c)

    return pairs(step)


def send(value, perm, name):
    with jax.named_scope(name):
        return lax.ppermute(value, AX, perm)


def gather_plane(own, flip, tag):
    p = lambda v, d, n: send(v, along(True, d, flip), tag + n)
    q = lambda v, d, n: send(v, along(False, d, flip), tag + n)
    v1, v2 = p(own, 1, "a"), p(own, -1, "b")
    w1, w2 = q(own, 1, "c"), q(own, -1, "d")
    u2 = p(own, 2, "e")
    s1, s2 = q(u2, 1, "f"), q(u2, -1, "g")
    a1, a2 = p(v1, 1, "h"), p(v1, -1, "i")
    b1, b2 = p(v2, 1, "j"), p(v2, -1, "k")
    f1 = p(w1, 1, "l")
    f2 = p(s2, -1, "m")
    f3 = q(a1, 1, "n")
    f4 = q(b2, -1, "o")
    return (own, v1, v2, w1, w2, u2, s1, s2, a1, a2, b1, b2, f1, f2, f3, f4)


def plane_index(flip):
    fs = lax.axis_index("fs")
    x, z = fs % 4, fs // 4
    even = ((x + z) % 2 == 0) != flip
    out = []
    for dp, dq in OFFSETS:
        tx = x + jnp.where(even, dp, dq)
        tz = z + jnp.where(even, dq, dp)
        out.append(((tz + 4) % 4) * 4 + (tx + 4) % 4)
    return jnp.stack(out).astype(jnp.int32)


HB = 256


def hidden_kernel(idx, pos, gt, vt, *refs):
    toks, shards = refs[:8], refs[8:24]
    out = refs[24]
    x, wg, wv, pg, pv, sem_x, sem_w = refs[25:]
    copies = []
    for j in range(16):
        at = pl.multiple_of(idx[j] * 128, 128)
        for k, w in enumerate((wg, wv)):
            c = pltpu.make_async_copy(
                shards[j].at[pl.ds(k * 128, 128), :], w.at[pl.ds(at, 128), :], sem_w.at[k, j]
            )
            c.start()
            copies.append(c)
    for j in range(8):
        at = pl.multiple_of(pos[j] * 128, 128)
        c = pltpu.make_async_copy(toks[j], x.at[pl.ds(at, 128), :], sem_x.at[j])
        c.start()
        copies.append(c)
    for c in copies:
        c.wait()
    zero = jnp.zeros((8, HB), F32)
    pg[0:8, :] = zero
    pv[0:8, :] = zero
    for n in range(768 // HB):
        cols = slice(n * HB, (n + 1) * HB)
        pg[8:, :] = jnp.dot(x[...], wg[:, cols], preferred_element_type=F32).astype(BF).astype(F32)
        pv[8:, :] = jnp.dot(x[...], wv[:, cols], preferred_element_type=F32).astype(BF).astype(F32)

        def rows(b, carry):
            at = pl.multiple_of(b * 128, 128)
            mixes = []
            for p, t in ((pg, gt), (pv, vt)):
                blk = p[pl.ds(at, 136), :]
                mixes.append(
                    t[0:1, cols] * blk[6:134] + t[1:2, cols] * blk[7:135] + t[2:3, cols] * blk[8:136]
                )
            gate, value = mixes
            gelu = 0.5 * gate * (1.0 + lax.erf(gate * 0.7071067811865476))
            out[b % 2, b // 2, :, cols] = (gelu * value).astype(BF)
            return carry

        lax.fori_loop(0, 8, rows, 0)


def hidden_call(idx, pos, gt, vt, toks, shards):
    return pl.pallas_call(
        hidden_kernel,
        out_shape=jax.ShapeDtypeStruct((2, 4, 128, 768), BF),
        in_specs=[SMEM, SMEM, VMEM, VMEM] + [ANY] * 24,
        out_specs=VMEM,
        scratch_shapes=[
            pltpu.VMEM((1024, 2048), BF),
            pltpu.VMEM((2048, 768), BF),
            pltpu.VMEM((2048, 768), BF),
            pltpu.VMEM((1032, HB), F32),
            pltpu.VMEM((1032, HB), F32),
            pltpu.SemaphoreType.DMA((8,)),
            pltpu.SemaphoreType.DMA((2, 16)),
        ],
        cost_estimate=pl.CostEstimate(
            flops=2 * 1024 * 2048 * 1536, bytes_accessed=12 * 2**20, transcendentals=0
        ),
        name="hidden",
    )(idx, pos, gt, vt, *toks, *shards)


def other_kernel(n, core, hid, *refs):
    shards, out = refs[:n], refs[n]
    w = jnp.concatenate([s[...] for s in shards], axis=1)
    h = hid[1 - core[0]].reshape(512, 768)
    out[...] = jnp.dot(h, w, preferred_element_type=F32).astype(BF)


def other_call(core, hid, shards):
    n = len(shards)
    return pl.pallas_call(
        functools.partial(other_kernel, n),
        out_shape=jax.ShapeDtypeStruct((512, n * 128), BF),
        in_specs=[SMEM] + [VMEM] * (n + 1),
        out_specs=VMEM,
        cost_estimate=pl.CostEstimate(
            flops=2 * 512 * 768 * n * 128, bytes_accessed=2 * 2**20, transcendentals=0
        ),
        name="other",
    )(core, hid, *shards)


def mine_kernel(n, core, hid, recv, *refs):
    shards, outs = refs[:n], refs[n:n + 4]
    acc = refs[n + 4]
    w = jnp.concatenate([s[...] for s in shards], axis=1)
    h = hid[core[0]].reshape(512, 768)
    acc[...] = jnp.dot(h, w, preferred_element_type=F32) + recv[...].astype(F32)
    for d in range(4):
        at = pl.multiple_of(((core[1] + d) % 4) * 128, 128)
        outs[d][...] = acc[pl.ds(at, 128), :].astype(BF)


def mine_call(core, hid, recv, shards):
    n = len(shards)
    return pl.pallas_call(
        functools.partial(mine_kernel, n),
        out_shape=[jax.ShapeDtypeStruct((128, n * 128), BF)] * 4,
        in_specs=[SMEM] + [VMEM] * (n + 2),
        out_specs=[VMEM] * 4,
        scratch_shapes=[pltpu.VMEM((512, n * 128), F32)],
        cost_estimate=pl.CostEstimate(
            flops=2 * 512 * 768 * n * 128, bytes_accessed=2 * 2**20, transcendentals=0
        ),
        name="mine",
    )(core, hid, recv, *shards)


def norm_kernel(groups, idx, gain, shift, *refs):
    parts, out = refs[:4 * len(groups)], refs[4 * len(groups)]
    sums = []
    for g in range(len(groups)):
        a, b, c, d = (r[...].astype(F32) for r in parts[4 * g:4 * g + 4])
        sums.append((a + b) + (c + d))
    total = sum(jnp.sum(s, axis=1, keepdims=True) for s in sums)
    average = total * (1.0 / 2048)
    sums = [s - average for s in sums]
    variance = sum(jnp.sum(s * s, axis=1, keepdims=True) for s in sums) * (1.0 / 2048)
    scale = lax.rsqrt(variance + 1e-05)
    for (start, count), s in zip(groups, sums):
        for j in range(count):
            at = pl.multiple_of(idx[start + j] * 128, 128)
            col = s[:, j * 128:(j + 1) * 128] * scale
            out[:, pl.ds(at, 128)] = (col * gain[:, pl.ds(at, 128)] + shift[:, pl.ds(at, 128)]).astype(BF)


def norm_call(groups, idx, gain, shift, parts):
    return pl.pallas_call(
        functools.partial(norm_kernel, groups),
        out_shape=jax.ShapeDtypeStruct((128, 2048), BF),
        in_specs=[SMEM] + [VMEM] * (2 + len(parts)),
        out_specs=VMEM,
        name="norm",
    )(idx, gain, shift, *parts)


GROUPS = ((0, 6), (6, 6), (12, 4))


def local(
    tokens, gate_weight, value_weight, gate_taps, value_taps, down_weight, norm_gain, norm_shift
):
    tp = lax.axis_index("tp")
    y, c = tp // 2, tp % 2
    over_y = lambda d: pairs(lambda x, y, z, c: (x, y + d, z, c))
    swap = pairs(lambda x, y, z, c: (x, y, z, 1 - c))

    both = jnp.concatenate([gate_weight, value_weight], axis=0)
    weights = gather_plane(both, False, "gv")
    mine = [tokens]
    for d in (1, -1, 2):
        mine.append(send(tokens, over_y(d), "tok%d" % d))
    theirs = [send(t, swap, "tokswap") for t in mine]
    rows = [(y - d + 4) % 4 for d in (0, 1, -1, 2)]
    pos = jnp.stack([r * 2 + c for r in rows] + [r * 2 + 1 - c for r in rows]).astype(jnp.int32)
    downs = gather_plane(down_weight, True, "dn")
    hid = hidden_call(plane_index(False), pos, gate_taps, value_taps, mine + theirs, weights)

    core = jnp.stack([c, y]).astype(jnp.int32)
    parts = []
    for start, count in GROUPS:
        shards = downs[start:start + count]
        recv = send(other_call(core, hid, shards), swap, "swap")
        outs = mine_call(core, hid, recv, shards)
        parts.append(outs[0])
        for d in (1, 2, 3):
            parts.append(send(outs[d], over_y(d), "rs%d" % d))
    return norm_call(
        GROUPS, plane_index(True), norm_gain.reshape(1, -1), norm_shift.reshape(1, -1), parts
    )


def solution(mesh):
    in_specs = (
        P(("fs", "tp"), None),
        P("fs", "tp"),
        P("fs", "tp"),
        P(None, "tp"),
        P(None, "tp"),
        P("tp", "fs"),
        P(),
        P(),
    )
    out_specs = P(("fs", "tp"), None)
    return jax.shard_map(local, mesh=mesh, in_specs=in_specs, out_specs=out_specs, check_vma=False)
```

```python
import functools

import jax
import jax.numpy as jnp
from jax import lax
from jax.experimental import pallas as pl
from jax.experimental.pallas import tpu as pltpu
from jax.sharding import PartitionSpec as P

AX = ("fs", "tp")
VMEM = pl.BlockSpec(memory_space=pltpu.VMEM)
BF = jnp.bfloat16
F32 = jnp.float32
MIB = 2**20

SIXTEEN = (
    (0, 0), (-1, 0), (1, 0), (2, 0), (0, -1), (-1, -1), (0, 1), (-1, 1),
    (1, -1), (2, -1), (1, 1), (2, 1), (0, 2), (-1, 2), (1, 2), (2, 2),
)
GROUPS = (
    ((0, 0), (-1, 0), (1, 0), (0, -1), (-1, -1), (1, -1), (0, 1), (-1, 1), (1, 1)),
    ((2, 0), (2, -1), (2, 1), (0, 2), (-1, 2), (1, 2), (2, 2)),
)
HELD = (
    ((0, 0), (0, 1), (0, 2), (1, 0), (1, 1), (1, 2), (2, 0), (2, 1), (2, 2)),
    ((0, 3), (1, 3), (2, 3), (3, 0), (3, 1), (3, 2), (3, 3)),
)
MIRROR = ((0, 3, 6, 1, 4, 7, 2, 5, 8), (3, 4, 5, 0, 1, 2, 6))
FORWARD = (True, True)


def pairs(step):
    out = []
    for z in range(4):
        for x in range(4):
            for y in range(4):
                for c in range(2):
                    tx, ty, tz, tc = step(x, y, z, c)
                    out.append((
                        (z * 4 + x) * 8 + y * 2 + c,
                        ((tz % 4) * 4 + tx % 4) * 8 + (ty % 4) * 2 + tc,
                    ))
    return out


def by_core(first, d):
    def step(x, y, z, c):
        return (x + d, y, z, c) if (c == 0) == first else (x, y, z + d, c)

    return pairs(step)


def turn(d):
    return pairs(lambda x, y, z, c: (x, y + (d if c == 0 else -d), z, c))


def send(value, perm):
    return lax.ppermute(value, AX, perm)


def swap(value):
    return send(value, pairs(lambda x, y, z, c: (x, y, z, 1 - c)))


def gather(both, down):
    p = lambda v, d: send(v, by_core(True, d))
    q = lambda v, d: send(v, by_core(False, d))
    a, b, e = p(both, 1), p(both, -1), p(both, 2)
    r, s = stack(both, a), stack(b, e)
    rp, rm, sp, sm = q(r, 1), q(r, -1), q(s, 1), q(s, -1)
    t = stack(down, p(down, 1), p(down, -1), p(down, 2))
    tp, tm = q(t, 1), q(t, -1)
    tf = q(tp, 1)
    return (r, s, rp, rm, sp, sm), (q(rp, 1), q(sm, -1)), (t, tp, tm, tf)


def stack_kernel(*refs):
    *ins, out = refs
    at = 0
    for r in ins:
        out[at:at + r.shape[0], :] = r[...]
        at += r.shape[0]


def stack(*arrays):
    rows, cols = sum(a.shape[0] for a in arrays), arrays[0].shape[1]
    return pl.pallas_call(
        stack_kernel,
        out_shape=jax.ShapeDtypeStruct((rows, cols), BF),
        in_specs=[VMEM] * len(arrays),
        out_specs=VMEM,
        compiler_params=pltpu.CompilerParams(vmem_limit_bytes=6 * MIB),
        name="stack",
    )(*arrays)


def place():
    fs, tp = lax.axis_index("fs"), lax.axis_index("tp")
    return lax.rem(fs, 4), tp // 2, fs // 4, lax.rem(tp, 2)


def column_block(offset, x, z, along_x):
    dp, dq = offset
    tx = lax.rem(x + 4 + jnp.where(along_x, dp, dq), 4)
    tz = lax.rem(z + 4 + jnp.where(along_x, dq, dp), 4)
    return pl.ds(pl.multiple_of((tz * 4 + tx) * 128, 128), 128)


def load(first, toks, bufs, xs, w):
    x, y, z, c = place()
    sign = 1 - 2 * c
    rows = [lax.rem(y + 4 - d * sign, 4) * 2 + c for d in (0, 1, -1, 2)]
    rows += [lax.rem(y + 4 + d * sign, 4) * 2 + 1 - c for d in (0, 1, -1, 2)]
    for k in range(2 * len(bufs)):
        at, row, buf = slice(k * 128, (k + 1) * 128), k % 2 * 256, bufs[k // 2]
        w[at, 0:768] = buf[row:row + 128, :]
        w[at, 768:1536] = buf[row + 128:row + 256, :]
        src = column_block(SIXTEEN[first + k], x, z, c == 0)
        for j in range(8):
            dst = pl.ds(pl.multiple_of(rows[j] * 128, 128), 128)
            xs[dst, at] = toks[j // 4][j % 4 * 128:(j % 4 + 1) * 128, src]


def early_kernel(*refs):
    toks, bufs = refs[:2], refs[2:-3]
    acc, x, w = refs[-3:]
    load(0, toks, bufs, x, w)
    acc[...] = jnp.dot(x[...], w[...], preferred_element_type=F32)


def early_call(toks, bufs):
    return pl.pallas_call(
        early_kernel,
        out_shape=jax.ShapeDtypeStruct((1024, 1536), F32),
        in_specs=[VMEM] * (2 + len(bufs)),
        out_specs=VMEM,
        scratch_shapes=[pltpu.VMEM((1024, 1536), BF), pltpu.VMEM((1536, 1536), BF)],
        cost_estimate=pl.CostEstimate(
            flops=2 * 1024 * 1536 * 1536, bytes_accessed=12 * MIB, transcendentals=0
        ),
        compiler_params=pltpu.CompilerParams(vmem_limit_bytes=32 * MIB),
        name="early",
    )(*toks, *bufs)


def hidden_kernel(gt, vt, acc, *refs):
    toks, bufs = refs[:2], refs[2:4]
    out, x, w, pre = refs[4:]
    load(12, toks, bufs, x, w)
    pre[0:8, :] = jnp.zeros((8, 1536), F32)
    for n in range(6):
        cols = slice(n * 256, (n + 1) * 256)
        total = acc[:, cols] + jnp.dot(x[...], w[:, cols], preferred_element_type=F32)
        pre[8:, cols] = total.astype(BF).astype(F32)

    def rows(b, carry):
        for n in range(3):
            for r in range(0, 128, 32):
                at = pl.multiple_of(b * 128 + r, 32)
                mixes = []
                for t, start in ((gt, 0), (vt, 768)):
                    cols = slice(n * 256, (n + 1) * 256)
                    blk = pre[pl.ds(at, 40), start + n * 256:start + (n + 1) * 256]
                    mixes.append(
                        t[0:1, cols] * blk[6:38] + t[1:2, cols] * blk[7:39] + t[2:3, cols] * blk[8:40]
                    )
                gate, value = mixes
                gelu = 0.5 * gate * (1.0 + lax.erf(gate * 0.7071067811865476))
                out[lax.rem(b, 2), b // 2, r:r + 32, cols] = (gelu * value).astype(BF)
        return carry

    lax.fori_loop(0, 8, rows, 0)


def hidden_call(gt, vt, acc, toks, bufs):
    return pl.pallas_call(
        hidden_kernel,
        out_shape=jax.ShapeDtypeStruct((2, 4, 128, 768), BF),
        in_specs=[VMEM] * (5 + len(bufs)),
        out_specs=VMEM,
        scratch_shapes=[
            pltpu.VMEM((1024, 512), BF),
            pltpu.VMEM((512, 1536), BF),
            pltpu.VMEM((1032, 1536), F32),
        ],
        cost_estimate=pl.CostEstimate(
            flops=2 * 1024 * 512 * 1536, bytes_accessed=12 * MIB, transcendentals=0
        ),
        compiler_params=pltpu.CompilerParams(vmem_limit_bytes=26 * MIB),
        name="hidden",
    )(gt, vt, acc, *toks, *bufs)


def columns(g, c, shards, w):
    for j, (buf, k) in enumerate(HELD[g]):
        at = pl.multiple_of((j + c * (MIRROR[g][j] - j)) * 128, 128)
        w[:, pl.ds(at, 128)] = shards[buf][k * 768:(k + 1) * 768, :]


def other_kernel(g, hid, *refs):
    *shards, out, w = refs
    _, _, _, c = place()
    columns(g, c, shards, w)
    h = hid[1 - c].reshape(512, 768)
    out[...] = jnp.dot(h, w[...], preferred_element_type=F32).astype(BF)


def other_call(g, hid, shards):
    n = len(GROUPS[g]) * 128
    return pl.pallas_call(
        functools.partial(other_kernel, g),
        out_shape=jax.ShapeDtypeStruct((512, n), BF),
        in_specs=[VMEM] * (1 + len(shards)),
        out_specs=VMEM,
        scratch_shapes=[pltpu.VMEM((768, n), BF)],
        cost_estimate=pl.CostEstimate(
            flops=2 * 512 * 768 * n, bytes_accessed=2 * MIB, transcendentals=0
        ),
        compiler_params=pltpu.CompilerParams(vmem_limit_bytes=12 * MIB),
        name="other",
    )(hid, *shards)


def mine_kernel(g, hid, recv, *refs):
    *shards, kept, ahead, far, behind, acc, w = refs
    _, y, _, c = place()
    columns(g, c, shards, w)
    h = hid[c].reshape(512, 768)
    acc[...] = jnp.dot(h, w[...], preferred_element_type=F32) + recv[...].astype(F32)
    sign = 1 - 2 * c
    for d, out in ((0, kept), (1, ahead), (2, far), (-1, behind)):
        at = pl.multiple_of(lax.rem(y + 4 + d * sign, 4) * 128, 128)
        out[...] = acc[pl.ds(at, 128), :].astype(out.dtype)


def mine_call(g, hid, recv, shards):
    n = len(GROUPS[g]) * 128
    types = (F32, F32 if FORWARD[g] else BF, BF, BF)
    return pl.pallas_call(
        functools.partial(mine_kernel, g),
        out_shape=[jax.ShapeDtypeStruct((128, n), t) for t in types],
        in_specs=[VMEM] * (2 + len(shards)),
        out_specs=[VMEM] * 4,
        scratch_shapes=[pltpu.VMEM((512, n), F32), pltpu.VMEM((768, n), BF)],
        cost_estimate=pl.CostEstimate(
            flops=2 * 512 * 768 * n, bytes_accessed=2 * MIB, transcendentals=0
        ),
        compiler_params=pltpu.CompilerParams(vmem_limit_bytes=14 * MIB),
        name="mine",
    )(hid, recv, *shards)


def add_kernel(a, b, out):
    out[...] = (a[...] + b[...].astype(F32)).astype(BF)


def add_call(a, b):
    return pl.pallas_call(
        add_kernel,
        out_shape=jax.ShapeDtypeStruct(a.shape, BF),
        in_specs=[VMEM] * 2,
        out_specs=VMEM,
        compiler_params=pltpu.CompilerParams(vmem_limit_bytes=4 * MIB),
        name="add",
    )(a, b)


def norm_kernel(counts, gain, shift, *refs):
    *parts, out = refs
    sums, at = [], 0
    for count in counts:
        sums.append(sum(p[...].astype(F32) for p in parts[at:at + count]))
        at += count
    total = sum(jnp.sum(s, axis=1, keepdims=True) for s in sums)
    average = total * (1.0 / 2048)
    sums = [s - average for s in sums]
    variance = sum(jnp.sum(s * s, axis=1, keepdims=True) for s in sums) * (1.0 / 2048)
    scale = lax.rsqrt(variance + 1e-05)
    x, _, z, _ = place()
    for steps, s in zip(GROUPS, sums):
        for j, step in enumerate(steps):
            at = column_block(step, x, z, True)
            col = s[:, j * 128:(j + 1) * 128] * scale
            out[:, at] = (col * gain[:, at] + shift[:, at]).astype(BF)


def norm_call(gain, shift, groups):
    parts = [p for g in groups for p in g]
    return pl.pallas_call(
        functools.partial(norm_kernel, [len(g) for g in groups]),
        out_shape=jax.ShapeDtypeStruct((128, 2048), BF),
        in_specs=[VMEM] * (2 + len(parts)),
        out_specs=VMEM,
        compiler_params=pltpu.CompilerParams(vmem_limit_bytes=12 * MIB),
        name="norm",
    )(gain, shift, *parts)


def layer(
    tokens, gate_weight, value_weight, gate_taps, value_taps, down_weight, norm_gain, norm_shift
):
    early, late, downs = gather(stack(gate_weight, value_weight), down_weight)
    mine = [tokens, send(tokens, turn(1)), send(tokens, turn(-1))]
    mine.append(send(mine[1], turn(1)))
    mine = stack(*mine)
    toks = (mine, swap(mine))
    acc = early_call(toks, early)
    hid = hidden_call(gate_taps, value_taps, acc, toks, late)

    groups = []
    for g, forward in enumerate(FORWARD):
        bufs = downs[:3 + g]
        sent = other_call(g, hid, bufs)
        recv = swap(sent)
        kept, ahead, far, behind = mine_call(g, hid, recv, bufs)
        parts = [kept, send(behind, turn(-1))]
        far = send(far, turn(1 if forward else 2))
        if forward:
            ahead = add_call(ahead, far)
        else:
            parts.append(far)
        parts.append(send(ahead, turn(1)))
        groups.append(parts)
    return norm_call(norm_gain.reshape(1, -1), norm_shift.reshape(1, -1), groups)


def solution(mesh):
    in_specs = (
        P(("fs", "tp"), None),
        P("fs", "tp"),
        P("fs", "tp"),
        P(None, "tp"),
        P(None, "tp"),
        P("tp", "fs"),
        P(),
        P(),
    )
    out_specs = P(("fs", "tp"), None)
    return jax.shard_map(layer, mesh=mesh, in_specs=in_specs, out_specs=out_specs, check_vma=False)
```

```python
import functools

import jax
import jax.numpy as jnp
from jax import lax
from jax.experimental import pallas as pl
from jax.experimental.pallas import tpu as pltpu
from jax.sharding import PartitionSpec as P

AX = ("fs", "tp")
VMEM = pl.BlockSpec(memory_space=pltpu.VMEM)
BF = jnp.bfloat16
F32 = jnp.float32
MIB = 2**20

SIXTEEN = (
    (0, 0), (-1, 0), (1, 0), (2, 0), (0, -1), (-1, -1), (0, 1), (-1, 1),
    (1, -1), (2, -1), (1, 1), (2, 1), (0, 2), (-1, 2), (1, 2), (2, 2),
)
DOWN = (
    ((0, 0), (-1, 0)), ((1, 0), (2, 0)), ((0, -1), (-1, -1)), ((1, 1), (2, 1)),
    ((1, -1), (2, -1)), ((1, 2), (2, 2)), ((0, 2), (-1, 2)), ((0, 1), (-1, 1)),
)
GROUPS = (
    ((0, 0), (-1, 0), (0, -1), (-1, -1), (1, 1), (2, 1), (1, 2), (2, 2)),
    ((1, 0), (0, 1), (2, 0), (0, 2), (1, -1), (-1, 1), (2, -1), (-1, 2)),
)
BUFFERS = (6, 8)
PARTS = (((2, -1), (1, 0)), ((2, -1, 1, 0),))


def pairs(step):
    out = []
    for z in range(4):
        for x in range(4):
            for y in range(4):
                for c in range(2):
                    tx, ty, tz, tc = step(x, y, z, c)
                    out.append((
                        (z * 4 + x) * 8 + y * 2 + c,
                        ((tz % 4) * 4 + tx % 4) * 8 + (ty % 4) * 2 + tc,
                    ))
    return out


def by_core(first, d):
    def step(x, y, z, c):
        return (x + d, y, z, c) if (c == 0) == first else (x, y, z + d, c)

    return pairs(step)


def turn(d):
    return pairs(lambda x, y, z, c: (x, y + (d if c == 0 else -d), z, c))


def send(value, perm):
    return lax.ppermute(value, AX, perm)


def swap(value):
    return send(value, pairs(lambda x, y, z, c: (x, y, z, 1 - c)))


def gather(both, down):
    p = lambda v, d: send(v, by_core(True, d))
    q = lambda v, d: send(v, by_core(False, d))
    a, b, e = p(both, 1), p(both, -1), p(both, 2)
    r, s = stack(both, a), stack(b, e)
    rp, rm, sp, sm = q(r, 1), q(r, -1), q(s, 1), q(s, -1)
    t = stack(down, p(down, 1))
    u = stack(p(down, -1), p(down, 2))
    tp, um = q(t, 1), q(u, -1)
    tf, uf = q(tp, 1), q(um, -1)
    up, tm = q(u, 1), q(t, -1)
    return (r, s, rp, rm, sp, sm), (q(rp, 1), q(sm, -1)), (t, u, tp, um, up, uf, tf, tm)


def stack_kernel(*refs):
    *ins, out = refs
    at = 0
    for r in ins:
        out[at:at + r.shape[0], :] = r[...]
        at += r.shape[0]


def stack(*arrays):
    rows, cols = sum(a.shape[0] for a in arrays), arrays[0].shape[1]
    return pl.pallas_call(
        stack_kernel,
        out_shape=jax.ShapeDtypeStruct((rows, cols), BF),
        in_specs=[VMEM] * len(arrays),
        out_specs=VMEM,
        compiler_params=pltpu.CompilerParams(vmem_limit_bytes=6 * MIB),
        name="stack",
    )(*arrays)


def place():
    fs, tp = lax.axis_index("fs"), lax.axis_index("tp")
    return lax.rem(fs, 4), tp // 2, fs // 4, lax.rem(tp, 2)


def column_block(offset, x, z, along_x):
    dp, dq = offset
    tx = lax.rem(x + 4 + jnp.where(along_x, dp, dq), 4)
    tz = lax.rem(z + 4 + jnp.where(along_x, dq, dp), 4)
    return pl.ds(pl.multiple_of((tz * 4 + tx) * 128, 128), 128)


def load(first, toks, bufs, xs, w):
    x, y, z, c = place()
    sign = 1 - 2 * c
    rows = [lax.rem(y + 4 - d * sign, 4) * 2 + c for d in (0, 1, -1, 2)]
    rows += [lax.rem(y + 4 + d * sign, 4) * 2 + 1 - c for d in (0, 1, -1, 2)]
    for k in range(2 * len(bufs)):
        at, row, buf = slice(k * 128, (k + 1) * 128), k % 2 * 256, bufs[k // 2]
        w[at, 0:768] = buf[row:row + 128, :]
        w[at, 768:1536] = buf[row + 128:row + 256, :]
        src = column_block(SIXTEEN[first + k], x, z, c == 0)
        for j in range(8):
            dst = pl.ds(pl.multiple_of(rows[j] * 128, 128), 128)
            xs[dst, at] = toks[j // 4][j % 4 * 128:(j % 4 + 1) * 128, src]


def early_kernel(*refs):
    toks, bufs = refs[:2], refs[2:-3]
    acc, x, w = refs[-3:]
    load(0, toks, bufs, x, w)
    acc[...] = jnp.dot(x[...], w[...], preferred_element_type=F32)


def early_call(toks, bufs):
    return pl.pallas_call(
        early_kernel,
        out_shape=jax.ShapeDtypeStruct((1024, 1536), F32),
        in_specs=[VMEM] * (2 + len(bufs)),
        out_specs=VMEM,
        scratch_shapes=[pltpu.VMEM((1024, 1536), BF), pltpu.VMEM((1536, 1536), BF)],
        cost_estimate=pl.CostEstimate(
            flops=2 * 1024 * 1536 * 1536, bytes_accessed=12 * MIB, transcendentals=0
        ),
        compiler_params=pltpu.CompilerParams(vmem_limit_bytes=32 * MIB),
        name="early",
    )(*toks, *bufs)


def hidden_kernel(gt, vt, acc, *refs):
    toks, bufs = refs[:2], refs[2:4]
    out, x, w, *pre = refs[4:]
    load(12, toks, bufs, x, w)
    for p in pre:
        p[0:8, :] = jnp.zeros((8, 256), F32)

    def multiply(n):
        for half in (0, 1):
            cols = slice(half * 768 + n * 256, half * 768 + (n + 1) * 256)
            total = acc[:, cols] + jnp.dot(x[...], w[:, cols], preferred_element_type=F32)
            pre[n % 2 * 2 + half][8:, :] = total.astype(BF).astype(F32)

    def combine(n):
        cols = slice(n * 256, (n + 1) * 256)
        taps = [t[:, cols] * 0.7071067811865476 for t in (gt, vt)]
        for at in range(0, 1024, 32):
            gate, value = (
                t[0:1] * p[at + 6:at + 38, :]
                + t[1:2] * p[at + 7:at + 39, :]
                + t[2:3] * p[at + 8:at + 40, :]
                for t, p in zip(taps, pre[n % 2 * 2:n % 2 * 2 + 2])
            )
            gelu = gate + gate * lax.erf(gate)
            b, r = at // 128, at % 128
            out[b % 2, b // 2, r:r + 32, cols] = (gelu * value).astype(BF)

    multiply(0)
    for n in range(3):
        if n < 2:
            multiply(n + 1)
        combine(n)


def hidden_call(gt, vt, acc, toks, bufs):
    return pl.pallas_call(
        hidden_kernel,
        out_shape=jax.ShapeDtypeStruct((2, 4, 128, 768), BF),
        in_specs=[VMEM] * (5 + len(bufs)),
        out_specs=VMEM,
        scratch_shapes=[
            pltpu.VMEM((1024, 512), BF),
            pltpu.VMEM((512, 1536), BF),
        ] + [pltpu.VMEM((1032, 256), F32)] * 4,
        cost_estimate=pl.CostEstimate(
            flops=2 * 1024 * 512 * 1536, bytes_accessed=12 * MIB, transcendentals=0
        ),
        compiler_params=pltpu.CompilerParams(vmem_limit_bytes=26 * MIB),
        name="hidden",
    )(gt, vt, acc, *toks, *bufs)


def columns(g, c, shards, w):
    for buf, offsets in zip(shards, DOWN):
        for k, (p, q) in enumerate(offsets):
            if (p, q) in GROUPS[g]:
                j, mirrored = GROUPS[g].index((p, q)), GROUPS[g].index((q, p))
                at = pl.multiple_of((j + c * (mirrored - j)) * 128, 128)
                w[:, pl.ds(at, 128)] = buf[k * 768:(k + 1) * 768, :]


def block(hid, c, steps):
    _, y, _, _ = place()
    at = [lax.rem(y + 4 + d * (1 - 2 * c), 4) for d in steps]
    return jnp.concatenate([hid[c, k] for k in at], axis=0)


def first_kernel(g, steps, hid, *refs):
    *shards, out, w = refs
    _, _, _, c = place()
    columns(g, c, shards, w)
    out[...] = jnp.dot(block(hid, 1 - c, steps), w[...], preferred_element_type=F32).astype(BF)


def other_kernel(steps, hid, w, out):
    _, _, _, c = place()
    out[...] = jnp.dot(block(hid, 1 - c, steps), w[...], preferred_element_type=F32).astype(BF)


def mine_kernel(steps, hid, w, recv, *outs):
    _, _, _, c = place()
    total = jnp.dot(block(hid, c, steps), w[...], preferred_element_type=F32)
    total = total + recv[...].astype(F32)
    for k, out in enumerate(outs):
        out[...] = total[k * 128:(k + 1) * 128].astype(out.dtype)


def product(kernel, rows, n, operands, outs):
    return pl.pallas_call(
        kernel,
        out_shape=outs,
        in_specs=[VMEM] * len(operands),
        out_specs=[VMEM] * len(outs),
        cost_estimate=pl.CostEstimate(
            flops=2 * rows * 768 * n, bytes_accessed=2 * MIB, transcendentals=0
        ),
        compiler_params=pltpu.CompilerParams(vmem_limit_bytes=14 * MIB),
        name="product",
    )(*operands)


def summed_over_core(g, hid, shards):
    n, sums, recv = len(GROUPS[g]) * 128, {}, []
    for i, steps in enumerate(PARTS[g]):
        rows = len(steps) * 128
        out = jax.ShapeDtypeStruct((rows, n), BF)
        if i == 0:
            kernel = functools.partial(first_kernel, g, steps)
            outs = [out, jax.ShapeDtypeStruct((768, n), BF)]
            sent, w = product(kernel, rows, n, (hid, *shards), outs)
        else:
            kernel = functools.partial(other_kernel, steps)
            (sent,) = product(kernel, rows, n, (hid, w), [out])
        recv.append(swap(sent))
    for i, steps in enumerate(PARTS[g]):
        outs = [jax.ShapeDtypeStruct((128, n), F32 if d in (0, 1) else BF) for d in steps]
        kernel = functools.partial(mine_kernel, steps)
        sums.update(zip(steps, product(kernel, len(steps) * 128, n, (hid, w, recv[i]), outs)))
    return sums


def add_kernel(a, b, out):
    out[...] = (a[...] + b[...].astype(F32)).astype(BF)


def add_call(a, b):
    return pl.pallas_call(
        add_kernel,
        out_shape=jax.ShapeDtypeStruct(a.shape, BF),
        in_specs=[VMEM] * 2,
        out_specs=VMEM,
        compiler_params=pltpu.CompilerParams(vmem_limit_bytes=4 * MIB),
        name="add",
    )(a, b)


def norm_kernel(counts, gain, shift, *refs):
    *parts, out = refs
    sums, at = [], 0
    for count in counts:
        sums.append(sum(p[...].astype(F32) for p in parts[at:at + count]))
        at += count
    total = sum(jnp.sum(s, axis=1, keepdims=True) for s in sums)
    average = total * (1.0 / 2048)
    sums = [s - average for s in sums]
    variance = sum(jnp.sum(s * s, axis=1, keepdims=True) for s in sums) * (1.0 / 2048)
    scale = lax.rsqrt(variance + 1e-05)
    x, _, z, _ = place()
    for steps, s in zip(GROUPS, sums):
        for j, step in enumerate(steps):
            at = column_block(step, x, z, True)
            col = s[:, j * 128:(j + 1) * 128] * scale
            out[:, at] = (col * gain[:, at] + shift[:, at]).astype(BF)


def norm_call(gain, shift, groups):
    parts = [p for g in groups for p in g]
    return pl.pallas_call(
        functools.partial(norm_kernel, [len(g) for g in groups]),
        out_shape=jax.ShapeDtypeStruct((128, 2048), BF),
        in_specs=[VMEM] * (2 + len(parts)),
        out_specs=VMEM,
        compiler_params=pltpu.CompilerParams(vmem_limit_bytes=12 * MIB),
        name="norm",
    )(gain, shift, *parts)


def layer(
    tokens, gate_weight, value_weight, gate_taps, value_taps, down_weight, norm_gain, norm_shift
):
    early, late, downs = gather(stack(gate_weight, value_weight), down_weight)
    mine = [tokens, send(tokens, turn(1)), send(tokens, turn(-1))]
    mine.append(send(mine[1], turn(1)))
    mine = stack(*mine)
    toks = (mine, swap(mine))
    acc = early_call(toks, early)
    hid = hidden_call(gate_taps, value_taps, acc, toks, late)

    groups = []
    for g, count in enumerate(BUFFERS):
        sums = summed_over_core(g, hid, downs[:count])
        behind = send(sums[-1], turn(-1))
        far = send(sums[2], turn(1))
        ahead = add_call(sums[1], far)
        groups.append((sums[0], behind, send(ahead, turn(1))))
    return norm_call(norm_gain.reshape(1, -1), norm_shift.reshape(1, -1), groups)


def solution(mesh):
    in_specs = (
        P(("fs", "tp"), None),
        P("fs", "tp"),
        P("fs", "tp"),
        P(None, "tp"),
        P(None, "tp"),
        P("tp", "fs"),
        P(),
        P(),
    )
    out_specs = P(("fs", "tp"), None)
    return jax.shard_map(layer, mesh=mesh, in_specs=in_specs, out_specs=out_specs, check_vma=False)
```
